32 devices in a mesh: ep: 8 (over z, y), tp: 4 (over x, core).
Axes of the slice: x: 2, y: 2, z: 4, core: 2. Of those that a mesh axis runs over, the one named last changes fastest.
Arguments:
- value_in: bfloat16 [4096, 1024], P('ep', 'tp'), may hold values from -6 to 6
- gate_in: bfloat16 [4096, 1024], P('ep', 'tp'), may hold values from -6 to 6
- outer_gate: bfloat16 [4096, 1024], P('ep', 'tp'), may hold values from -6 to 6
- conv_weight: bfloat16 [3, 1024], P(None, 'tp'), may hold values from -3.5 to 3.5
- out_weight: bfloat16 [1024, 2048], P('tp'), may hold values from -0.1875 to 0.1875
- moe_tokens: bfloat16 [4096, 2048], P(('ep', 'tp')), may hold values from -6 to 6
- norm_gain: bfloat16 [2048], replicated, may hold values from 0.099609375 to 1.8984375
- routes: int32 [4096, 2], P(('ep', 'tp')), may hold values from 0 to 7, all different within a row; in each aligned block of 128 rows (0 to 127, 128 to 255, ...) at most 48 rows name the same one
- route_weight: float32 [4096, 2], P(('ep', 'tp')), may hold values from 0.1 to 1
- expert_gate: bfloat16 [8, 2048, 6144], P('ep', None, 'tp'), may hold values from -0.125 to 0.125
- expert_up: bfloat16 [8, 2048, 6144], P('ep', None, 'tp'), may hold values from -0.125 to 0.125
- expert_down: bfloat16 [8, 6144, 2048], P('ep', 'tp'), may hold values from -0.078125 to 0.078125
Outputs:
- mixer_out: bfloat16 [4096, 2048], P(('ep', 'tp'))
- moe_out: bfloat16 [4096, 2048], P(('ep', 'tp'))
The draws below stay inside these ranges and needn't reach their ends.
Inputs may be any that keep to these rules, and one draw needn't show every extreme that they name: `routes`: each row names 2 different experts. Among the rows of one device no expert is named by more than 48 rows, a bound that some blocks reach.
All inputs are finite; a program needn't handle non-finite values.
Results may differ from the reference program's by a relative error of at most 0.012.
Values may be sent and summed in bfloat16 or wider, within the bound.
A program may use at most 128 MiB of HBM per device.

```python
import math
import jax
import jax.numpy as jnp
import numpy as np
from jax import lax

D = 2048
CW = 1024
FFE = 6144
TOP = 2
TOK_DEV = 128
EXPERTS = 8
CAP = 48
TOKENS_A = 4096
TOKENS_B = 4096
N_TP = 4


def levels(own_key, dims, cuts, smallest, largest):
    level = 1.0
    for axis_at, blocks in cuts:
        heights = jax.random.uniform(jax.random.fold_in(jax.random.fold_in(own_key, 6), axis_at), (blocks,), jnp.float32, smallest / len(cuts), largest / len(cuts))
        level = level * jnp.repeat(jnp.exp(heights), dims[axis_at] // blocks).reshape((-1,) + (1,) * (len(dims) - 1 - axis_at))
    return level


def shared_out(stream_key, own, number, rows, amount, top, most, lean):
    order = jax.random.permutation(stream_key, amount)
    packed, usual = load_shares(amount, rows * top, most, lean, True), load_shares(amount, rows * top, most, lean, False)
    places = jnp.arange(amount)

    def named(tallies, rotation):
        used = int((tallies > 0).sum())
        fixed = max(1, used // 4)
        moved = fixed + (places - fixed + rotation * (used - fixed)) % max(1, amount - fixed)
        return jnp.zeros((amount,), jnp.int32).at[order[jnp.where(places < fixed, places, moved)]].set(jnp.asarray(tallies, jnp.int32))

    tallies = jnp.where(number % 4 == 0, named(packed, number // 4), named(usual, number - number // 4 - 1))
    mixed = jax.random.permutation(jax.random.fold_in(own, 3), amount)
    donor, sink = mixed[0:amount // 2 * 2:2], mixed[1:amount // 2 * 2:2]
    margin = jnp.minimum(tallies[donor] - 1, most - tallies[sink]) // 2
    margin = jnp.where((donor == order[0]) | (sink == order[0]) | (tallies[sink] == 0), 0, jnp.maximum(margin, 0))
    moved = jax.random.randint(jax.random.fold_in(own, 4), (amount // 2,), 0, 1 << 20) % (margin + 1)
    tallies = tallies.at[donor].add(-moved).at[sink].add(moved)
    labels = jnp.searchsorted(jnp.cumsum(tallies), jnp.arange(rows * top), side="right").astype(jnp.int32)
    listing = labels.reshape(top, rows).T
    listing = listing[jax.random.permutation(jax.random.fold_in(own, 1), rows)]
    rotation = jax.random.randint(jax.random.fold_in(own, 2), (rows, 1), 0, top)
    return jnp.take_along_axis(listing, (jnp.arange(top)[None, :] + rotation) % top, axis=1)


def load_shares(number_of, total, reach, skew, full):
    loads = [(1 << 20) // math.isqrt(standing ** skew) + 1 for standing in range(1, number_of + 1)]
    largest = reach if full else min(reach, max(-(-total // number_of), total * loads[0] // sum(loads)))
    least = 1 if total - largest >= number_of - 1 else 0
    holding, spare = [largest] + [least] * (number_of - 1), total - largest - least * (number_of - 1)
    while spare > 0:
        candidates = [i for i in range(1, number_of) if holding[i] < largest] or [i for i in range(1, number_of) if holding[i] < reach]
        whole, budget = sum([loads[i] for i in candidates]), spare
        for i in candidates:
            more = min(reach - holding[i], max(1, budget * loads[i] // whole), spare)
            holding[i] = holding[i] + more
            spare = spare - more
    return np.array(holding)


def scatter_about(own_key, shape, deviation, bound, pieces=(), kind=jnp.bfloat16):
    loudness = levels(own_key, shape, pieces, -0.22, 0.18) if pieces else 1.0
    drawn = jax.random.normal(own_key, shape, jnp.float32) * deviation * loudness
    return jnp.minimum(jnp.maximum(drawn, -bound), bound).astype(kind)


def setup_inputs(seed: int = 0) -> dict:
    key_list = jax.random.split(jax.random.key(seed), 13)
    value_in = scatter_about(key_list[0], (TOKENS_A, CW), 1.0, 6.0, ((0, 8), (1, 4)))
    gate_in = scatter_about(key_list[1], (TOKENS_A, CW), 1.0, 6.0, ((0, 8), (1, 4)))
    outer_gate = scatter_about(key_list[2], (TOKENS_A, CW), 1.0, 6.0, ((0, 8), (1, 4)))
    conv_weight = scatter_about(key_list[3], (3, CW), 3 ** -0.5, 3.5, ((1, 4),))
    out_weight = scatter_about(key_list[4], (CW, D), CW ** -0.5, 0.1875, ((0, 4),))
    moe_tokens = scatter_about(key_list[5], (TOKENS_B, D), 1.0, 6.0, ((0, 32),))
    norm_gain = jnp.clip(1.0 + 0.18 * jax.random.normal(key_list[6], (D,), jnp.float32), 0.099609375, 1.8984375).astype(jnp.bfloat16)
    routes_keys = jax.random.split(jax.random.fold_in(key_list[7], 1), TOKENS_B // TOK_DEV)
    routes_turns = jax.random.permutation(jax.random.fold_in(key_list[7], 3), TOKENS_B // TOK_DEV)
    routes = jax.vmap(lambda own, number: shared_out(jax.random.fold_in(key_list[7], 2), own, number, TOK_DEV, EXPERTS, TOP, CAP, 2))(routes_keys, routes_turns).reshape((TOKENS_B, TOP))
    route_weight = jnp.clip(0.1 + 0.9 * jax.random.uniform(key_list[8], (TOKENS_B, TOP), jnp.float32) ** levels(key_list[8], (TOKENS_B, TOP), ((0, 32),), -0.2, 0.2), 0.1, 1.0)
    expert_gate = scatter_about(key_list[9], (EXPERTS, D, FFE), D ** -0.5, 0.125, ((0, 8), (2, 4)))
    expert_up = scatter_about(key_list[10], (EXPERTS, D, FFE), D ** -0.5, 0.125, ((0, 8), (2, 4)))
    expert_down = scatter_about(key_list[11], (EXPERTS, FFE, D), FFE ** -0.5, 0.078125, ((0, 8), (1, 4)))
    return {"value_in": value_in, "gate_in": gate_in, "outer_gate": outer_gate, "conv_weight": conv_weight, "out_weight": out_weight, "moe_tokens": moe_tokens, "norm_gain": norm_gain, "routes": routes, "route_weight": route_weight, "expert_gate": expert_gate, "expert_up": expert_up, "expert_down": expert_down}


def rounded(values):
    return lax.optimization_barrier(values.astype(jnp.bfloat16)).astype(jnp.float32)

def reference(value_in, gate_in, outer_gate, conv_weight, out_weight, moe_tokens, norm_gain, routes, route_weight, expert_gate, expert_up, expert_down):
    product = (value_in.astype(jnp.float32) * gate_in.astype(jnp.float32)).astype(jnp.bfloat16)
    padded = jnp.pad(product.astype(jnp.float32), ((1, 1), (0, 0)))
    taps = conv_weight.astype(jnp.float32)
    convolved = padded[:-2] * taps[0] + padded[1:-1] * taps[1] + padded[2:] * taps[2]
    mixed_rows = (outer_gate.astype(jnp.float32) * convolved).astype(jnp.bfloat16)
    group_width = CW // N_TP
    running = jnp.zeros((TOKENS_A, D), jnp.float32)
    for group in range(N_TP):
        partial_value = jnp.dot(mixed_rows[:, group * group_width:(group + 1) * group_width], out_weight[group * group_width:(group + 1) * group_width], preferred_element_type=jnp.float32)
        running = running + rounded(partial_value)
    mixer_out = running.astype(jnp.bfloat16)
    tokens_f32 = moe_tokens.astype(jnp.float32)
    normed = (tokens_f32 * lax.rsqrt(lax.optimization_barrier(jnp.mean(tokens_f32 * tokens_f32, axis=-1, keepdims=True)) + 1e-06) * norm_gain.astype(jnp.float32)).astype(jnp.bfloat16)
    devices = TOKENS_B // TOK_DEV
    flat_ids = routes.reshape(devices, TOK_DEV * TOP)
    matches = (flat_ids[..., None] == jnp.arange(EXPERTS, dtype=jnp.int32)[None, None, :]).astype(jnp.int32)
    position = lax.optimization_barrier(jnp.sum((jnp.cumsum(matches, axis=1) - 1) * matches, axis=-1)).astype(jnp.int32)
    owners = jnp.arange(devices, dtype=jnp.int32)[:, None]
    columns = (owners * CAP + position).astype(jnp.int32)
    token_ids = jnp.broadcast_to(jnp.arange(TOKENS_B, dtype=jnp.int32).reshape(devices, TOK_DEV, 1), (devices, TOK_DEV, TOP)).reshape(devices, TOK_DEV * TOP)
    slot_table = jnp.zeros((EXPERTS, devices * CAP), jnp.int32).at[flat_ids, columns].set(token_ids + 1)
    padded_rows = jnp.concatenate([jnp.zeros((1, D), jnp.bfloat16), normed], axis=0)
    unit_width = FFE // N_TP

    def expert(operands):
        indices, gate_w, up_w, down_w = operands
        picked_rows = padded_rows[indices]
        gate_act = jnp.dot(picked_rows, gate_w, preferred_element_type=jnp.float32)
        up_act = jnp.dot(picked_rows, up_w, preferred_element_type=jnp.float32)
        hidden = (jax.nn.silu(gate_act) * up_act).astype(jnp.bfloat16)
        summed = jnp.zeros((indices.shape[0], D), jnp.float32)
        for group in range(N_TP):
            partial_value = jnp.dot(hidden[:, group * unit_width:(group + 1) * unit_width], down_w[group * unit_width:(group + 1) * unit_width], preferred_element_type=jnp.float32)
            summed = summed + rounded(partial_value)
        return summed.astype(jnp.bfloat16)
    results = lax.map(expert, (slot_table, expert_gate, expert_up, expert_down))
    where_ids = (flat_ids * (devices * CAP) + columns).reshape(TOKENS_B, TOP)
    picked = results.reshape(EXPERTS * devices * CAP, D)[where_ids].astype(jnp.float32)
    moe_out = lax.optimization_barrier(jnp.sum(route_weight[..., None] * picked, axis=1)).astype(jnp.bfloat16)
    return (mixer_out, moe_out)
```

```python
import functools

import jax
import jax.numpy as jnp
from jax import lax
from jax.experimental import pallas as pl
from jax.experimental.pallas import tpu as pltpu
from jax.sharding import PartitionSpec as P


def extended(x, sides, width):
    for axis, dim in sides:
        size, length = (lax.axis_size(axis), x.shape[dim])
        up = [(i, (i + 1) % size) for i in range(size - 1)]
        down = [(j, i) for i, j in up]
        last = lax.slice_in_dim(x, length - width, length, axis=dim)
        leading = lax.slice_in_dim(x, 0, width, axis=dim)
        before = lax.ppermute(last, axis, up)
        after = lax.ppermute(leading, axis, down)
        x = jnp.concatenate([before, x, after], axis=dim)
    return x


def rounded(values):
    return lax.optimization_barrier(values.astype(jnp.bfloat16)).astype(jnp.float32)


def mixer_half(value_in, gate_in, outer_gate, conv_weight, out_weight):
    product = (value_in.astype(jnp.float32) * gate_in.astype(jnp.float32)).astype(jnp.bfloat16)
    padded = extended(product, (("ep", 0),), 1).astype(jnp.float32)
    taps = conv_weight.astype(jnp.float32)
    convolved = padded[:-2] * taps[0] + padded[1:-1] * taps[1] + padded[2:] * taps[2]
    mixed_rows = (outer_gate.astype(jnp.float32) * convolved).astype(jnp.bfloat16)
    return rounded(jnp.dot(mixed_rows, out_weight, preferred_element_type=jnp.float32)).astype(
        jnp.bfloat16
    )


MESH = pl.DeviceIdType.MESH


def expert_kernel(
    experts, shards, cap, tile,
    sent, gate_hbm, up_hbm, down_hbm, back,
    gate_w, up_w, down_w, slots, hidden, part, core_in, pair, chip_in, total,
    w_sem, own_sem, out_s, out_r, xf_s, xf_r, df_s, df_r, dr_s, dr_r, xr_s, xr_r, bk_s, bk_r,
):
    stages = experts // 2
    high = shards // 2
    me, mine = lax.axis_index("ep"), lax.axis_index("tp")
    low, top = lax.rem(mine, 2), mine // 2
    partner = (me, mine + 1 - 2 * low)
    across = (me, lax.rem(mine + high, shards))
    wide, half = 2 * cap, 2 * high * cap
    own_half = pl.multiple_of(low * half, 16)
    other_half = pl.multiple_of((1 - low) * half, 16)
    own_top = pl.multiple_of(top * wide, 16)
    other_top = pl.multiple_of((1 - top) * wide, 16)

    def to(k):
        return lax.rem(me + k, experts)

    def source(k):
        return lax.rem(me + experts - k, experts)

    def place(k):
        return pl.ds(pl.multiple_of(own_half + own_top + (k % 2) * cap, 16), cap)

    def remote(src, dst, s, r, device):
        return pltpu.make_async_remote_copy(
            src_ref=src, dst_ref=dst, send_sem=s, recv_sem=r, device_id=device, device_id_type=MESH
        )

    loads = [
        pltpu.make_async_copy(a, b, w_sem.at[i])
        for i, (a, b) in enumerate(((gate_hbm, gate_w), (up_hbm, up_w), (down_hbm, down_w)))
    ]
    barrier = pltpu.get_barrier_semaphore()
    for k in range(1, experts):
        pl.semaphore_signal(barrier, inc=1, device_id=(to(k), mine), device_id_type=MESH)
    for device in (partner, across):
        pl.semaphore_signal(barrier, inc=1, device_id=device, device_id_type=MESH)
    for load in loads:
        load.start()
    own_in = pltpu.make_async_copy(sent.at[me], slots.at[0, place(0)], own_sem.at[0])
    own_in.start()
    pl.semaphore_wait(barrier, experts + 1)

    out = [None] + [
        remote(sent.at[to(k)], slots.at[k // 2, place(k)], out_s.at[k], out_r.at[k], (to(k), mine))
        for k in range(1, experts)
    ]
    for copy in out[1:]:
        copy.start()
    x_out = [
        remote(slots.at[k // 2, place(k)], slots.at[k // 2, place(k)], xf_s.at[k], xf_r.at[k], across)
        for k in range(experts)
    ]
    rows = pl.ds(own_half, half)
    d_out = [
        remote(slots.at[j, rows], slots.at[j, rows], df_s.at[j], df_r.at[j], partner)
        for j in range(stages)
    ]
    d_back = [
        remote(part.at[j, pl.ds(other_half, half)], core_in.at[j], dr_s.at[j], dr_r.at[j], partner)
        for j in range(stages)
    ]
    x_back = [
        remote(pair.at[j, pl.ds(other_top, wide)], chip_in.at[j], xr_s.at[j], xr_r.at[j], across)
        for j in range(stages)
    ]
    own_out = pltpu.make_async_copy(total.at[0, pl.ds(0, cap)], back.at[me], own_sem.at[1])
    home = [own_out] + [
        remote(
            total.at[k // 2, pl.ds((k % 2) * cap, cap)], back.at[me], bk_s.at[k], bk_r.at[k],
            (source(k), mine),
        )
        for k in range(1, experts)
    ]

    def arrive(j):
        for k in (2 * j, 2 * j + 1):
            if k == 0:
                own_in.wait()
            else:
                out[k].wait_recv()
            x_out[k].start()

    def spread(j):
        x_out[2 * j].wait_recv()
        x_out[2 * j + 1].wait_recv()
        d_out[j].start()

    def activate(j):
        d_out[j].wait_recv()

        def step(i, carry):
            at = pl.ds(pl.multiple_of(i * tile, tile), tile)
            x = slots[j]
            g = jnp.dot(x, gate_w[:, at], preferred_element_type=jnp.float32)
            u = jnp.dot(x, up_w[:, at], preferred_element_type=jnp.float32)
            hidden[:, at] = (g / (1.0 + jnp.exp(-g)) * u).astype(jnp.bfloat16)
            return carry

        lax.fori_loop(0, gate_w.shape[1] // tile, step, 0)

    def project(j):
        def step(i, carry):
            at = pl.ds(pl.multiple_of(i * tile, tile), tile)
            part[j, :, at] = jnp.dot(
                hidden[...], down_w[:, at], preferred_element_type=jnp.float32
            ).astype(jnp.bfloat16)
            return carry

        lax.fori_loop(0, down_w.shape[1] // tile, step, 0)
        d_back[j].start()

    def pair_up(j):
        d_back[j].wait_recv()
        pair[j] = (
            part[j, pl.ds(own_half, half)].astype(jnp.float32) + core_in[j].astype(jnp.float32)
        ).astype(jnp.bfloat16)
        x_back[j].start()

    def finish(j):
        x_back[j].wait_recv()
        total[j] = (
            pair[j, pl.ds(own_top, wide)].astype(jnp.float32) + chip_in[j].astype(jnp.float32)
        ).astype(jnp.bfloat16)
        home[2 * j].start()
        home[2 * j + 1].start()

    arrive(0)
    spread(0)
    for j in range(stages):
        if j + 1 < stages:
            arrive(j + 1)
        if j == 0:
            loads[0].wait()
            loads[1].wait()
        activate(j)
        if j + 1 < stages:
            spread(j + 1)
        if j >= 1:
            pair_up(j - 1)
        if j >= 2:
            finish(j - 2)
        if j == 0:
            loads[2].wait()
        project(j)
    pair_up(stages - 1)
    if stages >= 2:
        finish(stages - 2)
    finish(stages - 1)
    own_out.wait()
    for k in range(1, experts):
        out[k].wait_send()
        home[k].wait()
    for k in range(experts):
        x_out[k].wait_send()
    for j in range(stages):
        d_out[j].wait_send()
        d_back[j].wait_send()
        x_back[j].wait_send()


def expert_half(
    partial_rows, moe_tokens, norm_gain, routes, route_weight, expert_gate, expert_up, expert_down
):
    row_total, top_count = routes.shape
    features = moe_tokens.shape[1]
    local_units = expert_gate.shape[2]
    experts, shards = lax.axis_size("ep"), lax.axis_size("tp")
    capacity = 3 * top_count * row_total // (2 * experts)
    capacity = -(-capacity // 16) * 16
    slots = experts * capacity
    tokens_f32 = moe_tokens.astype(jnp.float32)
    normed = (
        tokens_f32
        * lax.rsqrt(jnp.mean(tokens_f32 * tokens_f32, axis=-1, keepdims=True) + 1e-06)
        * norm_gain.astype(jnp.float32)
    ).astype(jnp.bfloat16)
    chosen = routes[:, :, None] == jnp.arange(experts, dtype=jnp.int32)[None, None, :]
    named = chosen.any(axis=1).astype(jnp.bfloat16)
    before = jnp.arange(row_total)[:, None] > jnp.arange(row_total)[None, :]
    rank = jnp.dot(before.astype(jnp.bfloat16), named, preferred_element_type=jnp.float32)
    position = jnp.sum(jnp.where(chosen, rank[:, None, :], 0.0), axis=2).astype(jnp.int32)
    slot_ids = routes * capacity + position
    at_slot = slot_ids[:, :, None] == jnp.arange(slots, dtype=jnp.int32)[None, None, :]
    placement = at_slot.any(axis=1).astype(jnp.bfloat16)
    outgoing = jnp.einsum("rs,rd->sd", placement, normed, preferred_element_type=jnp.float32)
    outgoing = outgoing.astype(jnp.bfloat16).reshape(experts, capacity, features)
    outgoing, partial_rows = lax.optimization_barrier((outgoing, partial_rows))
    mixer_out = lax.psum_scatter(partial_rows, "tp", scatter_dimension=0, tiled=True)
    stages, rows = experts // 2, 2 * shards * capacity
    bf16 = jnp.bfloat16
    dma = pltpu.SemaphoreType.DMA
    returned = pl.pallas_call(
        functools.partial(expert_kernel, experts, shards, capacity, 256),
        out_shape=jax.ShapeDtypeStruct((experts, capacity, features), bf16),
        in_specs=[pl.BlockSpec(memory_space=pltpu.VMEM)] + [pl.BlockSpec(memory_space=pl.ANY)] * 3,
        out_specs=pl.BlockSpec(memory_space=pltpu.VMEM),
        scratch_shapes=[
            pltpu.VMEM((features, local_units), bf16),
            pltpu.VMEM((features, local_units), bf16),
            pltpu.VMEM((local_units, features), bf16),
            pltpu.VMEM((stages, rows, features), bf16),
            pltpu.VMEM((rows, local_units), bf16),
            pltpu.VMEM((stages, rows, features), bf16),
            pltpu.VMEM((stages, rows // 2, features), bf16),
            pltpu.VMEM((stages, rows // 2, features), bf16),
            pltpu.VMEM((stages, rows // shards, features), bf16),
            pltpu.VMEM((stages, rows // shards, features), bf16),
            dma((3,)),
            dma((2,)),
        ]
        + [dma((experts,))] * 4
        + [dma((stages,))] * 6
        + [dma((experts,))] * 2,
        compiler_params=pltpu.CompilerParams(
            collective_id=0, has_side_effects=True, vmem_limit_bytes=60 * 2**20
        ),
        cost_estimate=pl.CostEstimate(
            flops=6 * stages * rows * features * local_units,
            bytes_accessed=6 * features * local_units,
            transcendentals=stages * rows * local_units,
        ),
    )(outgoing, expert_gate[0], expert_up[0], expert_down[0])
    weights = jnp.sum(jnp.where(at_slot, route_weight[:, :, None], 0.0), axis=1)
    leading = weights.astype(bf16)
    trailing = (weights - leading.astype(jnp.float32)).astype(bf16)
    result = returned.reshape(slots, features)
    moe_out = jnp.dot(leading, result, preferred_element_type=jnp.float32) + jnp.dot(
        trailing, result, preferred_element_type=jnp.float32
    )
    return mixer_out, moe_out.astype(bf16)


def body(
    value_in,
    gate_in,
    outer_gate,
    conv_weight,
    out_weight,
    moe_tokens,
    norm_gain,
    routes,
    route_weight,
    expert_gate,
    expert_up,
    expert_down,
):
    partial_rows = mixer_half(value_in, gate_in, outer_gate, conv_weight, out_weight)
    return expert_half(
        partial_rows,
        moe_tokens,
        norm_gain,
        routes,
        route_weight,
        expert_gate,
        expert_up,
        expert_down,
    )


def solution(mesh):
    placed = (
        P("ep", "tp"),
        P("ep", "tp"),
        P("ep", "tp"),
        P(None, "tp"),
        P("tp", None),
        P(("ep", "tp"), None),
        P(),
        P(("ep", "tp"), None),
        P(("ep", "tp"), None),
        P("ep", None, "tp"),
        P("ep", None, "tp"),
        P("ep", "tp", None),
    )
    return jax.shard_map(
        body,
        mesh=mesh,
        in_specs=placed,
        out_specs=(P(("ep", "tp"), None), P(("ep", "tp"), None)),
        check_vma=False,
    )
```

```python
import functools

import jax
import jax.numpy as jnp
from jax import lax
from jax.experimental import pallas as pl
from jax.experimental.pallas import tpu as pltpu
from jax.sharding import PartitionSpec as P


def extended(x, sides, width):
    for axis, dim in sides:
        size, length = (lax.axis_size(axis), x.shape[dim])
        up = [(i, (i + 1) % size) for i in range(size - 1)]
        down = [(j, i) for i, j in up]
        last = lax.slice_in_dim(x, length - width, length, axis=dim)
        leading = lax.slice_in_dim(x, 0, width, axis=dim)
        before = lax.ppermute(last, axis, up)
        after = lax.ppermute(leading, axis, down)
        x = jnp.concatenate([before, x, after], axis=dim)
    return x


def rounded(values):
    return lax.optimization_barrier(values.astype(jnp.bfloat16)).astype(jnp.float32)


def mixer_half(value_in, gate_in, outer_gate, conv_weight, out_weight):
    product = (value_in.astype(jnp.float32) * gate_in.astype(jnp.float32)).astype(jnp.bfloat16)
    padded = extended(product, (("ep", 0),), 1).astype(jnp.float32)
    taps = conv_weight.astype(jnp.float32)
    convolved = padded[:-2] * taps[0] + padded[1:-1] * taps[1] + padded[2:] * taps[2]
    mixed_rows = (outer_gate.astype(jnp.float32) * convolved).astype(jnp.bfloat16)
    return rounded(jnp.dot(mixed_rows, out_weight, preferred_element_type=jnp.float32)).astype(
        jnp.bfloat16
    )


MESH = pl.DeviceIdType.MESH


def expert_kernel(
    experts, shards, cap, tile,
    sent, gate_hbm, up_hbm, down_hbm, back,
    gate_w, up_w, down_w, slots, hidden, part, core_in, pair, chip_in, total,
    w_sem, own_sem, out_s, out_r, xf_s, xf_r, df_s, df_r, dr_s, dr_r, xr_s, xr_r, bk_s, bk_r,
):
    stages = experts // 2
    high = shards // 2
    me, mine = lax.axis_index("ep"), lax.axis_index("tp")
    low, top = lax.rem(mine, 2), mine // 2
    partner = (me, mine + 1 - 2 * low)
    across = (me, lax.rem(mine + high, shards))
    wide, half = 2 * cap, 2 * high * cap
    own_half = pl.multiple_of(low * half, 16)
    other_half = pl.multiple_of((1 - low) * half, 16)
    own_top = pl.multiple_of(top * wide, 16)
    other_top = pl.multiple_of((1 - top) * wide, 16)

    def to(k):
        return lax.rem(me + k, experts)

    def source(k):
        return lax.rem(me + experts - k, experts)

    def place(k):
        return pl.ds(pl.multiple_of(own_half + own_top + (k % 2) * cap, 16), cap)

    def remote(src, dst, s, r, device):
        return pltpu.make_async_remote_copy(
            src_ref=src, dst_ref=dst, send_sem=s, recv_sem=r, device_id=device, device_id_type=MESH
        )

    loads = [
        pltpu.make_async_copy(a, b, w_sem.at[i])
        for i, (a, b) in enumerate(((gate_hbm, gate_w), (up_hbm, up_w), (down_hbm, down_w)))
    ]
    barrier = pltpu.get_barrier_semaphore()
    for k in range(1, experts):
        pl.semaphore_signal(barrier, inc=1, device_id=(to(k), mine), device_id_type=MESH)
    for device in (partner, across):
        pl.semaphore_signal(barrier, inc=1, device_id=device, device_id_type=MESH)
    for load in loads:
        load.start()
    own_in = pltpu.make_async_copy(sent.at[me], slots.at[0, place(0)], own_sem.at[0])
    own_in.start()
    pl.semaphore_wait(barrier, experts + 1)

    out = [None] + [
        remote(sent.at[to(k)], slots.at[k // 2, place(k)], out_s.at[k], out_r.at[k], (to(k), mine))
        for k in range(1, experts)
    ]
    for copy in out[1:]:
        copy.start()
    x_out = [
        remote(slots.at[k // 2, place(k)], slots.at[k // 2, place(k)], xf_s.at[k], xf_r.at[k], across)
        for k in range(experts)
    ]
    rows = pl.ds(own_half, half)
    d_out = [
        remote(slots.at[j, rows], slots.at[j, rows], df_s.at[j], df_r.at[j], partner)
        for j in range(stages)
    ]
    d_back = [
        remote(part.at[j, pl.ds(other_half, half)], core_in.at[j], dr_s.at[j], dr_r.at[j], partner)
        for j in range(stages)
    ]
    x_back = [
        remote(
            pair.at[k // 2, pl.ds(pl.multiple_of(other_top + (k % 2) * cap, 16), cap)],
            chip_in.at[k // 2, pl.ds((k % 2) * cap, cap)], xr_s.at[k], xr_r.at[k], across,
        )
        for k in range(experts)
    ]
    own_out = pltpu.make_async_copy(total.at[0, pl.ds(0, cap)], back.at[me], own_sem.at[1])
    home = [own_out] + [
        remote(
            total.at[k // 2, pl.ds((k % 2) * cap, cap)], back.at[me], bk_s.at[k], bk_r.at[k],
            (source(k), mine),
        )
        for k in range(1, experts)
    ]

    def arrive(j):
        for k in (2 * j, 2 * j + 1):
            if k == 0:
                own_in.wait()
            else:
                out[k].wait_recv()
            x_out[k].start()

    def spread(j):
        x_out[2 * j].wait_recv()
        x_out[2 * j + 1].wait_recv()
        d_out[j].start()

    def activate(j):
        d_out[j].wait_recv()

        def step(i, carry):
            at = pl.ds(pl.multiple_of(i * tile, tile), tile)
            x = slots[j]
            g = jnp.dot(x, gate_w[:, at], preferred_element_type=jnp.float32)
            u = jnp.dot(x, up_w[:, at], preferred_element_type=jnp.float32)
            hidden[:, at] = (g / (1.0 + jnp.exp(-g)) * u).astype(jnp.bfloat16)
            return carry

        lax.fori_loop(0, gate_w.shape[1] // tile, step, 0)

    def project(j):
        def step(i, carry):
            at = pl.ds(pl.multiple_of(i * tile, tile), tile)
            part[j, :, at] = jnp.dot(
                hidden[...], down_w[:, at], preferred_element_type=jnp.float32
            ).astype(jnp.bfloat16)
            return carry

        lax.fori_loop(0, down_w.shape[1] // tile, step, 0)
        d_back[j].start()

    def add_pair(j, first, count):
        mine_rows = pl.ds(pl.multiple_of(own_half + first, 16), count)
        pair[j, pl.ds(first, count)] = (
            part[j, mine_rows].astype(jnp.float32)
            + core_in[j, pl.ds(first, count)].astype(jnp.float32)
        ).astype(jnp.bfloat16)

    def pair_up(j):
        d_back[j].wait_recv()
        for k in (2 * j, 2 * j + 1):
            add_pair(j, pl.multiple_of(other_top + (k % 2) * cap, 16), cap)
            x_back[k].start()
        add_pair(j, own_top, wide)

    def finish(j):
        for k in (2 * j, 2 * j + 1):
            x_back[k].wait_recv()
            here = pl.ds((k % 2) * cap, cap)
            held = pl.ds(pl.multiple_of(own_top + (k % 2) * cap, 16), cap)
            total[j, here] = (
                pair[j, held].astype(jnp.float32) + chip_in[j, here].astype(jnp.float32)
            ).astype(jnp.bfloat16)
            home[k].start()

    arrive(0)
    spread(0)
    for j in range(stages):
        if j + 1 < stages:
            arrive(j + 1)
        if j == 0:
            loads[0].wait()
            loads[1].wait()
        activate(j)
        if j + 1 < stages:
            spread(j + 1)
        if j >= 1:
            pair_up(j - 1)
        if j >= 2:
            finish(j - 2)
        if j == 0:
            loads[2].wait()
        project(j)
    pair_up(stages - 1)
    if stages >= 2:
        finish(stages - 2)
    finish(stages - 1)
    own_out.wait()
    for k in range(1, experts):
        out[k].wait_send()
        home[k].wait()
    for k in range(experts):
        x_out[k].wait_send()
        x_back[k].wait_send()
    for j in range(stages):
        d_out[j].wait_send()
        d_back[j].wait_send()


def expert_half(
    partial_rows, moe_tokens, norm_gain, routes, route_weight, expert_gate, expert_up, expert_down
):
    row_total, top_count = routes.shape
    features = moe_tokens.shape[1]
    local_units = expert_gate.shape[2]
    experts, shards = lax.axis_size("ep"), lax.axis_size("tp")
    capacity = 3 * top_count * row_total // (2 * experts)
    capacity = -(-capacity // 16) * 16
    slots = experts * capacity
    tokens_f32 = moe_tokens.astype(jnp.float32)
    normed = (
        tokens_f32
        * lax.rsqrt(jnp.mean(tokens_f32 * tokens_f32, axis=-1, keepdims=True) + 1e-06)
        * norm_gain.astype(jnp.float32)
    ).astype(jnp.bfloat16)
    chosen = routes[:, :, None] == jnp.arange(experts, dtype=jnp.int32)[None, None, :]
    named = chosen.any(axis=1).astype(jnp.bfloat16)
    before = jnp.arange(row_total)[:, None] > jnp.arange(row_total)[None, :]
    rank = jnp.dot(before.astype(jnp.bfloat16), named, preferred_element_type=jnp.float32)
    position = jnp.sum(jnp.where(chosen, rank[:, None, :], 0.0), axis=2).astype(jnp.int32)
    slot_ids = routes * capacity + position
    at_slot = slot_ids[:, :, None] == jnp.arange(slots, dtype=jnp.int32)[None, None, :]
    placement = at_slot.any(axis=1).astype(jnp.bfloat16)
    outgoing = jnp.einsum("rs,rd->sd", placement, normed, preferred_element_type=jnp.float32)
    outgoing = outgoing.astype(jnp.bfloat16).reshape(experts, capacity, features)
    outgoing, partial_rows = lax.optimization_barrier((outgoing, partial_rows))
    mixer_out = lax.psum_scatter(partial_rows, "tp", scatter_dimension=0, tiled=True)
    stages, rows = experts // 2, 2 * shards * capacity
    bf16 = jnp.bfloat16
    dma = pltpu.SemaphoreType.DMA
    returned = pl.pallas_call(
        functools.partial(expert_kernel, experts, shards, capacity, 512),
        out_shape=jax.ShapeDtypeStruct((experts, capacity, features), bf16),
        in_specs=[pl.BlockSpec(memory_space=pltpu.VMEM)] + [pl.BlockSpec(memory_space=pl.ANY)] * 3,
        out_specs=pl.BlockSpec(memory_space=pltpu.VMEM),
        scratch_shapes=[
            pltpu.VMEM((features, local_units), bf16),
            pltpu.VMEM((features, local_units), bf16),
            pltpu.VMEM((local_units, features), bf16),
            pltpu.VMEM((stages, rows, features), bf16),
            pltpu.VMEM((rows, local_units), bf16),
            pltpu.VMEM((stages, rows, features), bf16),
            pltpu.VMEM((stages, rows // 2, features), bf16),
            pltpu.VMEM((stages, rows // 2, features), bf16),
            pltpu.VMEM((stages, rows // shards, features), bf16),
            pltpu.VMEM((stages, rows // shards, features), bf16),
            dma((3,)),
            dma((2,)),
        ]
        + [dma((experts,))] * 4
        + [dma((stages,))] * 4
        + [dma((experts,))] * 4,
        compiler_params=pltpu.CompilerParams(
            collective_id=0, has_side_effects=True, vmem_limit_bytes=60 * 2**20
        ),
        cost_estimate=pl.CostEstimate(
            flops=6 * stages * rows * features * local_units,
            bytes_accessed=6 * features * local_units,
            transcendentals=stages * rows * local_units,
        ),
    )(outgoing, expert_gate[0], expert_up[0], expert_down[0])
    weights = jnp.sum(jnp.where(at_slot, route_weight[:, :, None], 0.0), axis=1)
    leading = weights.astype(bf16)
    trailing = (weights - leading.astype(jnp.float32)).astype(bf16)
    result = returned.reshape(slots, features)
    moe_out = jnp.dot(leading, result, preferred_element_type=jnp.float32) + jnp.dot(
        trailing, result, preferred_element_type=jnp.float32
    )
    return mixer_out, moe_out.astype(bf16)


def body(
    value_in,
    gate_in,
    outer_gate,
    conv_weight,
    out_weight,
    moe_tokens,
    norm_gain,
    routes,
    route_weight,
    expert_gate,
    expert_up,
    expert_down,
):
    partial_rows = mixer_half(value_in, gate_in, outer_gate, conv_weight, out_weight)
    return expert_half(
        partial_rows,
        moe_tokens,
        norm_gain,
        routes,
        route_weight,
        expert_gate,
        expert_up,
        expert_down,
    )


def solution(mesh):
    placed = (
        P("ep", "tp"),
        P("ep", "tp"),
        P("ep", "tp"),
        P(None, "tp"),
        P("tp", None),
        P(("ep", "tp"), None),
        P(),
        P(("ep", "tp"), None),
        P(("ep", "tp"), None),
        P("ep", None, "tp"),
        P("ep", None, "tp"),
        P("ep", "tp", None),
    )
    return jax.shard_map(
        body,
        mesh=mesh,
        in_specs=placed,
        out_specs=(P(("ep", "tp"), None), P(("ep", "tp"), None)),
        check_vma=False,
    )
```
